32 devices in a mesh: grp: 2 (over y), sp: 8 (over z, core), tp: 2 (over x).
Axes of the slice: x: 2, y: 2, z: 4, core: 2. Of those that a mesh axis runs over, the one named last changes fastest.
Arguments:
- queries_a: bfloat16 [4096, 2, 512], P(('grp', 'sp'), None, 'tp'), parts along dimension 0, may hold values from -120 to 120
- keys_a: bfloat16 [4096, 2, 512], P(('grp', 'sp'), None, 'tp'), parts along dimension 0, may hold values from -6 to 6
- values_a: bfloat16 [4096, 1024], P(('grp', 'sp'), 'tp'), parts along dimension 0, may hold values from -6 to 6
- queries_b: bfloat16 [4096, 2, 512], P(('grp', 'sp'), None, 'tp'), parts along dimension 0, may hold values from -120 to 120
- keys_b: bfloat16 [4096, 2, 512], P(('grp', 'sp'), None, 'tp'), parts along dimension 0, may hold values from -6 to 6
- values_b: bfloat16 [4096, 1024], P(('grp', 'sp'), 'tp'), parts along dimension 0, may hold values from -6 to 6
- lambdas: float32 [12], replicated, may hold values from 0.3 to 0.8
- head_gain_a: float32 [256], replicated, may hold values from 0.1 to 1.9
- head_gain_b: float32 [128], replicated, may hold values from 0.1 to 1.9
- out_a: bfloat16 [1024, 2048], P('tp'), may hold values from -0.125 to 0.125
- out_b: bfloat16 [1024, 2048], P('tp'), may hold values from -0.125 to 0.125
- residual: bfloat16 [4096, 2048], P(('grp', 'sp', 'tp')), parts along dimension 0, may hold values from -6 to 6
- gain_mix: float32 [2048], replicated, may hold values from 0.1 to 1.9
- gain_pre: float32 [2048], replicated, may hold values from 0.1 to 1.9
- gain_post: float32 [2048], replicated, may hold values from 0.1 to 1.9
- routes: int32 [4096, 4], P(('grp', 'sp', 'tp')), parts along dimension 0, may hold values from 0 to 7, all different within a row; in each aligned block of 128 rows (0 to 127, 128 to 255, ...) at most 80 rows name the same one
- route_weights: float32 [4096, 4], P(('grp', 'sp', 'tp')), parts along dimension 0, may hold values from 0.05 to 1
- expert_gate: bfloat16 [8, 2048, 2048], P('sp', None, 'tp'), may hold values from -1 to 1
- expert_up: bfloat16 [8, 2048, 2048], P('sp', None, 'tp'), may hold values from -1 to 1
- expert_down: bfloat16 [8, 2048, 2048], P('sp', 'tp'), may hold values from -0.125 to 0.125
Outputs:
- layer_out: bfloat16 [4096, 2048], P(('grp', 'sp', 'tp')), parts along dimension 0
The draws below stay inside these ranges and needn't reach their ends.
There are 2 independent parts, one for each index of `grp`. The reference program is written for one: setup_inputs(seed, part) draws one part's arguments, and reference() takes and returns one part's arrays. A program takes and returns all parts, laid end to end along the dimension named above; an argument that names none is the same for every part. Nothing has to cross between parts.
Inputs may be any that keep to these rules, and one draw needn't show every extreme that they name: `routes`: in each aligned block of 128 rows (the rows of one device) no expert is named by more than 80 rows, a bound that some blocks reach.
All inputs are finite; a program needn't handle non-finite values.
Results may differ from the reference program's by a relative error of at most 0.018.
Values may be sent and summed in bfloat16 or wider, within the bound.
A program may use at most 128 MiB of HBM per device.

```python
import math
import jax
import jax.numpy as jnp
import numpy as np
from jax import lax

HA = 4
HB = 8
DA = 128
DB = 64
D = 2048
FF = 2048
TOP_K = 4
TOK_DEV = 256
TOKENS = 2048
TOKSUB = 128
EXPERTS = 8
CAP = 80
N_TP = 2


def pair_fields(key, salt, width):
    keys = jnp.clip(jax.random.normal(jax.random.fold_in(key, salt), (TOKENS, 2, width), jnp.float32) * 1.32, -6.0, 6.0)
    queries = jnp.clip(jax.random.normal(jax.random.fold_in(key, salt + 1), (TOKENS, 2, width), jnp.float32) * 1.32, -6.0, 6.0)
    return (queries, keys)


def draw_queries_a(key, part):
    queries, keys = pair_fields(key, 11, HA * DA)
    return queries.astype(jnp.bfloat16)


def draw_keys_a(key, part):
    queries, keys = pair_fields(key, 11, HA * DA)
    return keys.astype(jnp.bfloat16)


def draw_queries_b(key, part):
    queries, keys = pair_fields(key, 21, HB * DB)
    return queries.astype(jnp.bfloat16)


def draw_keys_b(key, part):
    queries, keys = pair_fields(key, 21, HB * DB)
    return keys.astype(jnp.bfloat16)


def expert_field(key, salt):
    base = jnp.clip(jax.random.normal(jax.random.fold_in(key, salt), (EXPERTS, D, FF), jnp.float32), -6.0, 6.0)
    factor = 1.0
    return jnp.clip(base * factor / jnp.sqrt(jnp.float32(D)), -1.0, 1.0)


def draw_expert_gate(key, part):
    return expert_field(key, 31).astype(jnp.bfloat16)


def draw_expert_up(key, part):
    return expert_field(key, 37).astype(jnp.bfloat16)


def block_scale(key, dims, cuts, smallest, high):
    def one(position, parts):
        heights = jax.random.uniform(jax.random.fold_in(jax.random.fold_in(key, 6), position), (parts,), jnp.float32, smallest / len(cuts), high / len(cuts))
        return jnp.repeat(jnp.exp(heights), dims[position] // parts).reshape((-1,) + (1,) * (len(dims) - position - 1))

    loudness = one(*cuts[0])
    for cut in cuts[1:]:
        loudness = loudness * one(*cut)
    return loudness


def assign_block(key, own, number, rows, amount, top, most, skew):
    ranking = jax.random.permutation(key, amount)
    packed, common = load_shares(amount, rows * top, most, skew, True), load_shares(amount, rows * top, most, skew, False)
    places = jnp.arange(amount)

    def named(lengths, rotation):
        used = int((lengths > 0).sum())
        fixed = max(1, used // 4)
        moved = fixed + (places - fixed + rotation * (used - fixed)) % max(1, amount - fixed)
        return jnp.zeros((amount,), jnp.int32).at[ranking[jnp.where(places < fixed, places, moved)]].set(jnp.asarray(lengths, jnp.int32))

    lengths = jnp.where(number % 4 == 0, named(packed, number // 4), named(common, number - number // 4 - 1))
    mixed = jax.random.permutation(jax.random.fold_in(own, 3), amount)
    source_of, sink = mixed[0:amount // 2 * 2:2], mixed[1:amount // 2 * 2:2]
    room = jnp.minimum(lengths[source_of] - 1, most - lengths[sink]) // 2
    room = jnp.where((source_of == ranking[0]) | (sink == ranking[0]) | (lengths[sink] == 0), 0, jnp.maximum(room, 0))
    moved = jax.random.randint(jax.random.fold_in(own, 4), (amount // 2,), 0, 1 << 20) % (room + 1)
    lengths = lengths.at[source_of].add(-moved).at[sink].add(moved)
    items = jnp.searchsorted(jnp.cumsum(lengths), jnp.arange(rows * top), side="right").astype(jnp.int32)
    grid = items.reshape(top, rows).T
    grid = grid[jax.random.permutation(jax.random.fold_in(own, 1), rows)]
    rotation = jax.random.randint(jax.random.fold_in(own, 2), (rows, 1), 0, top)
    return jnp.take_along_axis(grid, (jnp.arange(top)[None, :] + rotation) % top, axis=1)


def load_shares(amount, total, limit, lean, full):
    weights = [(1 << 20) // math.isqrt(standing ** lean) + 1 for standing in range(1, amount + 1)]
    largest = limit if full else min(limit, max(-(-total // amount), total * weights[0] // sum(weights)))
    least = 1 if total - largest >= amount - 1 else 0
    given, spare = [largest] + [least] * (amount - 1), total - largest - least * (amount - 1)
    while spare > 0:
        candidates = [i for i in range(1, amount) if given[i] < largest] or [i for i in range(1, amount) if given[i] < limit]
        pool, budget = sum([weights[i] for i in candidates]), spare
        for i in candidates:
            extra = min(limit - given[i], max(1, budget * weights[i] // pool), spare)
            given[i] = given[i] + extra
            spare = spare - extra
    return np.array(given)


def centred(stream_key, dims, deviation, most, split=(), kind=jnp.bfloat16):
    drawn = jax.random.normal(stream_key, dims, jnp.float32) * deviation
    if len(split) > 0:
        drawn = block_scale(stream_key, dims, split, -0.22, 0.18) * drawn
    return jnp.clip(drawn, min=-most, max=most).astype(kind)


def setup_inputs(seed: int = 0, part: int = 0) -> dict:
    seeds = jax.random.split(jax.random.key(seed), 21)
    part_splits = jax.random.split(jax.random.fold_in(seeds[20], part), 21)
    queries_a = draw_queries_a(jax.random.fold_in(jax.random.fold_in(seeds[20], part), 71), part)
    keys_a = draw_keys_a(jax.random.fold_in(jax.random.fold_in(seeds[20], part), 71), part)
    values_a = centred(part_splits[2], (TOKENS, HA * 2 * DA), 1.0, 6.0, ((0, 8), (1, 2)))
    queries_b = draw_queries_b(jax.random.fold_in(jax.random.fold_in(seeds[20], part), 71), part)
    keys_b = draw_keys_b(jax.random.fold_in(jax.random.fold_in(seeds[20], part), 71), part)
    values_b = centred(part_splits[5], (TOKENS, HB * 2 * DB), 1.0, 6.0, ((0, 8), (1, 2)))
    lambdas = jnp.clip(jax.random.uniform(seeds[6], (HA + HB,), jnp.float32, 0.3, 0.8), 0.3, 0.8)
    head_gain_a = jnp.clip(1.0 + 0.18 * jax.random.normal(seeds[7], (2 * DA,), jnp.float32), 0.1, 1.9)
    head_gain_b = jnp.clip(1.0 + 0.18 * jax.random.normal(seeds[8], (2 * DB,), jnp.float32), 0.1, 1.9)
    out_a = centred(seeds[9], (HA * 2 * DA, D), D ** -0.5, 0.125, ((0, 2),))
    out_b = centred(seeds[10], (HB * 2 * DB, D), D ** -0.5, 0.125, ((0, 2),))
    residual = centred(part_splits[11], (TOKENS, D), 1.0, 6.0, ((0, 16),))
    gain_mix = jnp.clip(1.0 + 0.18 * jax.random.normal(seeds[12], (D,), jnp.float32), 0.1, 1.9)
    gain_pre = jnp.clip(1.0 + 0.18 * jax.random.normal(seeds[13], (D,), jnp.float32), 0.1, 1.9)
    gain_post = jnp.clip(1.0 + 0.18 * jax.random.normal(seeds[14], (D,), jnp.float32), 0.1, 1.9)
    routes_keys = jax.random.split(jax.random.fold_in(part_splits[15], 1), TOKENS // TOKSUB)
    routes_turns = jax.random.permutation(jax.random.fold_in(part_splits[15], 3), TOKENS // TOKSUB)
    routes = jax.vmap(lambda own, number: assign_block(jax.random.fold_in(part_splits[15], 2), own, number, TOKSUB, EXPERTS, TOP_K, CAP, 1))(routes_keys, routes_turns).reshape((TOKENS, TOP_K))
    route_weights = jnp.clip(0.05 + 0.95 * jax.random.uniform(part_splits[16], (TOKENS, TOP_K), jnp.float32) ** block_scale(part_splits[16], (TOKENS, TOP_K), ((0, 16),), -0.2, 0.2), 0.05, 1.0)
    expert_gate = draw_expert_gate(jax.random.fold_in(seeds[20], 71), part)
    expert_up = draw_expert_up(jax.random.fold_in(seeds[20], 71), part)
    expert_down = centred(seeds[19], (EXPERTS, FF, D), FF ** -0.5, 0.125, ((0, 8), (1, 2)))
    return dict(queries_a=queries_a, keys_a=keys_a, values_a=values_a, queries_b=queries_b, keys_b=keys_b, values_b=values_b, lambdas=lambdas, head_gain_a=head_gain_a, head_gain_b=head_gain_b, out_a=out_a, out_b=out_b, residual=residual, gain_mix=gain_mix, gain_pre=gain_pre, gain_post=gain_post, routes=routes, route_weights=route_weights, expert_gate=expert_gate, expert_up=expert_up, expert_down=expert_down)


def rms_norm(values, gain_vec):
    return values * lax.rsqrt(lax.optimization_barrier(jnp.mean(values * values, -1, keepdims=True)) + 1e-06) * gain_vec.astype(jnp.float32)

def attend_group(queries, keys, values, weights_two, gain_vec, head_size):
    heads = queries.shape[2] // head_size
    query_all = queries.astype(jnp.float32).reshape(TOKENS, 2, heads, head_size)
    key_all = keys.astype(jnp.float32).reshape(TOKENS, 2, heads, head_size)
    value_all = values.astype(jnp.float32).reshape(TOKENS, heads, 2 * head_size)
    span_rows = 512 if TOKENS % 512 == 0 else TOKENS
    key_pos = jnp.arange(TOKENS, dtype=jnp.int32)

    def one_block(first_row):
        query_rows = lax.dynamic_slice_in_dim(query_all, first_row, span_rows, 0)
        query_pos = first_row + jnp.arange(span_rows, dtype=jnp.int32)
        visible = (key_pos[None, :] <= query_pos[:, None])[None, :, None, :]
        scores = jnp.einsum('qmhd,kmhd->mqhk', query_rows, key_all, precision=lax.Precision.HIGHEST) * head_size ** (-0.5)
        scores = jnp.where(visible, scores, -1e+30)
        row_top = lax.optimization_barrier(jnp.max(scores, -1, keepdims=True))
        exp_terms = jnp.where(visible, jnp.exp(scores - row_top), 0.0)
        totals = lax.optimization_barrier(jnp.sum(exp_terms, -1))
        rounded = lax.optimization_barrier(exp_terms.astype(jnp.bfloat16)).astype(jnp.float32)
        accum = jnp.einsum('mqhk,khe->mqhe', rounded, value_all, precision=lax.Precision.HIGHEST)
        mixture = accum[0] / totals[0][..., None] - weights_two[None, :, None] * accum[1] / totals[1][..., None]
        normed = rms_norm(mixture, gain_vec)
        return normed.reshape(span_rows, heads * 2 * head_size).astype(jnp.bfloat16)
    firsts = jnp.arange(0, TOKENS, span_rows, dtype=jnp.int32)
    return lax.map(one_block, firsts).reshape(TOKENS, heads * 2 * head_size)

def slot_numbers(flat_ids):
    onehot = (flat_ids[:, None] == jnp.arange(EXPERTS, dtype=jnp.int32)[None, :]).astype(jnp.int32)
    before = jnp.cumsum(onehot, 0) - onehot
    return lax.optimization_barrier(jnp.sum(before * onehot, 1)).astype(jnp.int32)

def reference(queries_a, keys_a, values_a, queries_b, keys_b, values_b, lambdas, head_gain_a, head_gain_b, out_a, out_b, residual, gain_mix, gain_pre, gain_post, routes, route_weights, expert_gate, expert_up, expert_down):
    heads_out_a = attend_group(queries_a, keys_a, values_a, lambdas[:HA], head_gain_a, DA)
    heads_out_b = attend_group(queries_b, keys_b, values_b, lambdas[HA:], head_gain_b, DB)
    width_a = heads_out_a.shape[1] // N_TP
    width_b = heads_out_b.shape[1] // N_TP
    mixed_rows = jnp.zeros((TOKENS, D), jnp.float32)
    for part_index in range(N_TP):
        part_a = jnp.dot(heads_out_a[:, part_index * width_a:(part_index + 1) * width_a], out_a[part_index * width_a:(part_index + 1) * width_a], preferred_element_type=jnp.float32)
        part_b = jnp.dot(heads_out_b[:, part_index * width_b:(part_index + 1) * width_b], out_b[part_index * width_b:(part_index + 1) * width_b], preferred_element_type=jnp.float32)
        mixed_rows = mixed_rows + lax.optimization_barrier((part_a + part_b).astype(jnp.bfloat16)).astype(jnp.float32)
    after_mix = (residual.astype(jnp.float32) + rms_norm(mixed_rows, gain_mix)).astype(jnp.bfloat16)
    normed = rms_norm(after_mix.astype(jnp.float32), gain_pre).astype(jnp.bfloat16)
    sub_rows = TOK_DEV // N_TP
    blocks = TOKENS // sub_rows
    route_blocks = routes.astype(jnp.int32).reshape(blocks, sub_rows * TOP_K)
    slot_ids = jax.vmap(slot_numbers)(route_blocks)
    block_ids = jnp.broadcast_to(jnp.arange(blocks, dtype=jnp.int32)[:, None], route_blocks.shape)
    token_ids = jnp.repeat(jnp.arange(TOKENS, dtype=jnp.int32).reshape(blocks, sub_rows), TOP_K, axis=1)
    table = jnp.full((EXPERTS, blocks, CAP), TOKENS, jnp.int32).at[route_blocks, block_ids, slot_ids].set(token_ids)
    padded = jnp.concatenate([normed, jnp.zeros((1, D), jnp.bfloat16)], 0)
    hidden_block = FF // N_TP

    def expert_work(expert_id):
        rows = padded[table[expert_id].reshape(-1)]
        gate_pre = jnp.dot(rows, expert_gate[expert_id], preferred_element_type=jnp.float32)
        up_pre = jnp.dot(rows, expert_up[expert_id], preferred_element_type=jnp.float32)
        glu_part = jnp.minimum(gate_pre, 7.0)
        lin_part = jnp.clip(up_pre, -7.0, 7.0)
        hidden = (glu_part * jax.nn.sigmoid(1.702 * glu_part) * (lin_part + 1.0)).astype(jnp.bfloat16)
        summed = jnp.zeros((rows.shape[0], D), jnp.float32)
        for part_index in range(N_TP):
            piece_sum = jnp.dot(hidden[:, part_index * hidden_block:(part_index + 1) * hidden_block], expert_down[expert_id][part_index * hidden_block:(part_index + 1) * hidden_block], preferred_element_type=jnp.float32)
            summed = summed + lax.optimization_barrier(piece_sum.astype(jnp.bfloat16)).astype(jnp.float32)
        return summed.astype(jnp.bfloat16).reshape(blocks, CAP, D)
    outputs = lax.map(expert_work, jnp.arange(EXPERTS, dtype=jnp.int32))
    picked = outputs[route_blocks, block_ids, slot_ids].astype(jnp.float32)
    weighted = picked * route_weights.reshape(blocks, sub_rows * TOP_K)[..., None].astype(jnp.float32)
    routed = lax.optimization_barrier(jnp.sum(weighted.reshape(TOKENS, TOP_K, D), 1))
    return (after_mix.astype(jnp.float32) + rms_norm(routed, gain_post)).astype(jnp.bfloat16)
```

```python
import jax
import jax.numpy as jnp
from jax import lax
from jax.experimental import pallas as pl
from jax.experimental.pallas import tpu as pltpu
from jax.sharding import PartitionSpec as P

HA = 4
DA = 128
DB = 64


def rms_norm(values, gain_vec):
    return values * lax.rsqrt(jnp.mean(values * values, -1, keepdims=True) + 1e-06) * gain_vec


def attend(current, query_rows, key_rows, value_rows, first_row, query_pos, head_size):
    run_max, run_sum, run_acc = current
    key_count = key_rows.shape[0]
    heads = query_rows.shape[2]
    key_view = key_rows.reshape(key_count, 2, heads, head_size)
    value_view = value_rows.reshape(key_count, heads, 2 * head_size)
    key_pos = first_row + jnp.arange(key_count, dtype=jnp.int32)
    visible = (key_pos[None, :] <= query_pos[:, None])[None, :, None, :]
    scores = jnp.einsum(
        "qmhd,kmhd->mqhk", query_rows, key_view, preferred_element_type=jnp.float32
    ) * head_size ** (-0.5)
    scores = jnp.where(visible, scores, -1e30)
    new_max = jnp.maximum(run_max, jnp.max(scores, -1))
    exp_terms = jnp.where(visible, jnp.exp(scores - new_max[..., None]), 0.0)
    rescale = jnp.exp(run_max - new_max)
    run_sum = run_sum * rescale + jnp.sum(exp_terms, -1)
    run_acc = run_acc * rescale[..., None] + jnp.einsum(
        "mqhk,khe->mqhe",
        exp_terms.astype(jnp.bfloat16),
        value_view,
        preferred_element_type=jnp.float32,
    )
    return (new_max, run_sum, run_acc)


def fresh_state(length, heads, head_size):
    return (
        jnp.full((2, length, heads), -1e30, jnp.float32),
        jnp.zeros((2, length, heads), jnp.float32),
        jnp.zeros((2, length, heads, 2 * head_size), jnp.float32),
    )


def finish(current, weights_two, gain_vec):
    run_max, run_sum, run_acc = current
    mixture = (
        run_acc[0] / run_sum[0][..., None]
        - weights_two[None, :, None] * run_acc[1] / run_sum[1][..., None]
    )
    normed = rms_norm(mixture, gain_vec)
    return normed.reshape(normed.shape[0], -1).astype(jnp.bfloat16)


MESH = pl.DeviceIdType.MESH
CORES = 2
VMEM_BYTES = 60 * 1024 * 1024


def place():
    sp = lax.axis_index("sp")
    return sp // CORES, sp % CORES, lax.axis_index("tp")


def greet(chips, tps):
    chip, core, tp = place()
    barrier = pltpu.get_barrier_semaphore()
    for step in range(1, chips):
        other = (chip + step) % chips
        pl.semaphore_signal(
            barrier, inc=1, device_id={"sp": other * CORES + core, "tp": tp}, device_id_type=MESH
        )
    for step in range(1, tps):
        pl.semaphore_signal(
            barrier,
            inc=1,
            device_id={"sp": chip * CORES + core, "tp": (tp + step) % tps},
            device_id_type=MESH,
        )
    pl.semaphore_signal(
        barrier, inc=1, device_id={"sp": chip * CORES + 1 - core, "tp": tp}, device_id_type=MESH
    )
    pl.semaphore_wait(barrier, chips - 1 + tps - 1 + 1)


def gather_kernel(chips, tps, own_ref, all_ref, send_sem, recv_sem, own_sem):
    chip, core, tp = place()
    greet(chips, tps)
    started = []

    def block(chip_of, core_of, tp_of):
        return (chip_of * CORES + core_of) * tps + tp_of

    def send(source, index, sp_to, tp_to):
        copy = pltpu.make_async_remote_copy(
            src_ref=source,
            dst_ref=all_ref.at[index],
            send_sem=send_sem.at[len(started)],
            recv_sem=recv_sem.at[index],
            device_id={"sp": sp_to, "tp": tp_to},
            device_id_type=MESH,
        )
        copy.start()
        started.append(copy)

    def arrived(index):
        pltpu.make_async_copy(all_ref.at[index], all_ref.at[index], recv_sem.at[index]).wait()

    own = block(chip, core, tp)
    for step in range(1, chips):
        send(own_ref, own, (chip + step) % chips * CORES + core, tp)
    for step in range(1, tps):
        send(own_ref, own, chip * CORES + core, (tp + step) % tps)
    send(own_ref, own, chip * CORES + 1 - core, tp)
    mine = pltpu.make_async_copy(own_ref, all_ref.at[own], own_sem)
    mine.start()

    def from_tp(chip_of):
        for step in range(1, tps):
            index = block(chip_of, core, (tp + step) % tps)
            arrived(index)
            send(all_ref.at[index], index, chip * CORES + 1 - core, tp)

    for step in range(1, chips):
        chip_of = (chip - step + chips) % chips
        index = block(chip_of, core, tp)
        arrived(index)
        for tp_step in range(1, tps):
            send(all_ref.at[index], index, chip * CORES + core, (tp + tp_step) % tps)
        send(all_ref.at[index], index, chip * CORES + 1 - core, tp)
        from_tp((chip - step + 1 + chips) % chips)
    from_tp((chip + 1) % chips)
    for step in range(chips):
        for tp_of in range(tps):
            arrived(block((chip - step + chips) % chips, 1 - core, (tp + tp_of) % tps))
    mine.wait()
    for copy in started:
        copy.wait_send()


def gather_rows(own, chips, tps):
    blocks = chips * CORES * tps
    sends = chips - 1 + tps - 1 + 1 + (chips - 1) * tps + chips * (tps - 1)
    return pl.pallas_call(
        lambda *refs: gather_kernel(chips, tps, *refs),
        name="gather_rows",
        out_shape=jax.ShapeDtypeStruct((blocks,) + own.shape, own.dtype),
        in_specs=[pl.BlockSpec(memory_space=pl.ANY)],
        out_specs=pl.BlockSpec(memory_space=pl.ANY),
        scratch_shapes=[
            pltpu.SemaphoreType.DMA((sends,)),
            pltpu.SemaphoreType.DMA((blocks,)),
            pltpu.SemaphoreType.DMA,
        ],
        compiler_params=pltpu.CompilerParams(collective_id=1, has_side_effects=True),
    )(own)


def add_rows(target, index, source, source_index):
    rows = target.shape[1]
    chunk = min(rows, 16)

    @pl.loop(0, rows // chunk)
    def _(part):
        span = pl.ds(pl.multiple_of(part * chunk, chunk), chunk)
        target[index, span, :] = (
            target[index, span, :].astype(jnp.float32)
            + source[source_index, span, :].astype(jnp.float32)
        ).astype(target.dtype)


def scatter_kernel(
    chips, tps, part_ref, out_ref, acc, core_in, tp_in, chip_in, load_sem, send_sem, core_sem, tp_sem, chip_sem
):
    chip, core, tp = place()
    load = []
    started = []
    for step in range(chips):
        for tp_step in range(tps):
            chip_of, tp_of = (chip + 1 + step) % chips, (tp + 1 + tp_step) % tps
            copy = pltpu.make_async_copy(
                part_ref.at[(chip_of * CORES + core) * tps + tp_of],
                acc.at[chip_of * tps + tp_of],
                load_sem.at[step * tps + tp_step],
            )
            copy.start()
            load.append(copy)
    greet(chips, tps)

    def send(source, target, recv_sem, sp_to, tp_to):
        copy = pltpu.make_async_remote_copy(
            src_ref=source,
            dst_ref=target,
            send_sem=send_sem.at[len(started)],
            recv_sem=recv_sem,
            device_id={"sp": sp_to, "tp": tp_to},
            device_id_type=MESH,
        )
        copy.start()
        started.append(copy)

    def arrived(target, index, sem):
        pltpu.make_async_copy(target.at[index], target.at[index], sem).wait()

    for step in range(chips):
        chip_of = (chip + 1 + step) % chips
        for tp_step in range(tps):
            tp_of = (tp + 1 + tp_step) % tps
            index = chip_of * tps + tp_of
            send(
                part_ref.at[(chip_of * CORES + 1 - core) * tps + tp_of],
                core_in.at[index],
                core_sem.at[index],
                chip * CORES + 1 - core,
                tp,
            )

    def chip_stage(step):
        chip_of = (chip + 1 + step) % chips
        for tp_step in range(1, tps):
            source = (tp + tp_step) % tps
            index = chip_of * tps + source
            arrived(tp_in, index, tp_sem.at[index])
            add_rows(acc, chip_of * tps + tp, tp_in, index)
        if step < chips - 1:
            send(
                acc.at[chip_of * tps + tp],
                chip_in.at[chip],
                chip_sem.at[chip],
                chip_of * CORES + core,
                tp,
            )

    for step in range(chips):
        chip_of = (chip + 1 + step) % chips
        for tp_step in range(tps):
            tp_of = (tp + 1 + tp_step) % tps
            index = chip_of * tps + tp_of
            load[step * tps + tp_step].wait()
            arrived(core_in, index, core_sem.at[index])
            add_rows(acc, index, core_in, index)
            if tp_step < tps - 1:
                send(
                    acc.at[index],
                    tp_in.at[chip_of * tps + tp],
                    tp_sem.at[chip_of * tps + tp],
                    chip * CORES + core,
                    tp_of,
                )
        if step > 0:
            chip_stage(step - 1)
    chip_stage(chips - 1)
    for step in range(1, chips):
        source = (chip - step + chips) % chips
        arrived(chip_in, source, chip_sem.at[source])
        if step < chips - 1:
            add_rows(acc, chip * tps + tp, chip_in, source)
    last = (chip + 1) % chips
    rows = out_ref.shape[0]
    chunk = min(rows, 16)

    @pl.loop(0, rows // chunk)
    def _(part):
        span = pl.ds(pl.multiple_of(part * chunk, chunk), chunk)
        out_ref[span, :] = acc[chip * tps + tp, span, :].astype(jnp.float32) + chip_in[
            last, span, :
        ].astype(jnp.float32)

    for copy in started:
        copy.wait_send()


def scatter_rows(parts, chips, tps):
    blocks, rows, width = parts.shape
    half = chips * tps
    sends = half + chips * (tps - 1) + chips - 1
    return pl.pallas_call(
        lambda *refs: scatter_kernel(chips, tps, *refs),
        name="scatter_rows",
        out_shape=jax.ShapeDtypeStruct((rows, width), jnp.float32),
        in_specs=[pl.BlockSpec(memory_space=pl.ANY)],
        out_specs=pl.BlockSpec(memory_space=pltpu.VMEM),
        scratch_shapes=[
            pltpu.VMEM((half, rows, width), parts.dtype),
            pltpu.VMEM((half, rows, width), parts.dtype),
            pltpu.VMEM((half, rows, width), parts.dtype),
            pltpu.VMEM((chips, rows, width), parts.dtype),
            pltpu.SemaphoreType.DMA((half,)),
            pltpu.SemaphoreType.DMA((sends,)),
            pltpu.SemaphoreType.DMA((half,)),
            pltpu.SemaphoreType.DMA((half,)),
            pltpu.SemaphoreType.DMA((chips,)),
        ],
        compiler_params=pltpu.CompilerParams(
            collective_id=2, has_side_effects=True, vmem_limit_bytes=VMEM_BYTES
        ),
    )(parts)


def expert_parts(gathered, expert, experts, capacity, width, weights):
    gate, up, down = weights
    blocks, rows, _ = gathered.shape
    shares = lax.dynamic_slice_in_dim(gathered[:, :, width:], expert, 1, 2)[:, :, 0]
    named = shares > 0
    order = jnp.arange(rows, dtype=jnp.int32)
    slots = jnp.dot(
        named.astype(jnp.bfloat16),
        (order[:, None] < order[None, :]).astype(jnp.bfloat16),
        preferred_element_type=jnp.float32,
    ).astype(jnp.int32)
    picks = (slots[:, None, :] == jnp.arange(capacity, dtype=jnp.int32)[None, :, None]) & named[:, None, :]
    rows_in = jnp.einsum(
        "bct,btd->bcd",
        picks.astype(jnp.bfloat16),
        gathered[:, :, :width],
        preferred_element_type=jnp.float32,
    ).astype(jnp.bfloat16)
    rows_in = rows_in.reshape(blocks * capacity, width)
    gate_pre = jnp.dot(rows_in, gate, preferred_element_type=jnp.float32)
    up_pre = jnp.dot(rows_in, up, preferred_element_type=jnp.float32)
    glu_part = jnp.minimum(gate_pre, 7.0)
    lin_part = jnp.clip(up_pre, -7.0, 7.0)
    hidden = (glu_part * jax.nn.sigmoid(1.702 * glu_part) * (lin_part + 1.0)).astype(jnp.bfloat16)
    outs = jnp.dot(hidden, down, preferred_element_type=jnp.float32).astype(jnp.bfloat16)
    back = jnp.where(picks, shares[:, None, :], 0).astype(jnp.bfloat16)
    return jnp.einsum(
        "bct,bcd->btd",
        back,
        outs.reshape(blocks, capacity, width),
        preferred_element_type=jnp.float32,
    ).astype(jnp.bfloat16)


def per_device(
    queries_a,
    keys_a,
    values_a,
    queries_b,
    keys_b,
    values_b,
    lambdas,
    head_gain_a,
    head_gain_b,
    out_a,
    out_b,
    residual,
    gain_mix,
    gain_pre,
    gain_post,
    routes,
    route_weights,
    expert_gate,
    expert_up,
    expert_down,
):
    length = queries_a.shape[0]
    heads_a = queries_a.shape[2] // DA
    heads_b = queries_b.shape[2] // DB
    head_slot = lax.axis_index("tp")
    seq_slot = lax.axis_index("sp")
    lambda_a = lax.dynamic_slice_in_dim(lambdas, head_slot * heads_a, heads_a)
    lambda_b = lax.dynamic_slice_in_dim(lambdas, HA + head_slot * heads_b, heads_b)
    groups = [
        (
            queries_a.reshape(length, 2, heads_a, DA),
            queries_b.reshape(length, 2, heads_b, DB),
            seq_slot * length + jnp.arange(length, dtype=jnp.int32),
            seq_slot * length + length - 1,
        )
    ]
    initial = tuple(
        (
            (
                fresh_state(group[2].shape[0], heads_a, DA),
                fresh_state(group[2].shape[0], heads_b, DB),
            )
            for group in groups
        )
    )
    pieces = (
        lax.all_gather(keys_a, "sp", axis=0, tiled=True),
        lax.all_gather(values_a, "sp", axis=0, tiled=True),
        lax.all_gather(keys_b, "sp", axis=0, tiled=True),
        lax.all_gather(values_b, "sp", axis=0, tiled=True),
    )
    key_count = pieces[0].shape[0]
    span_rows = 1024

    def one_span(span_index, carried):
        offset = span_index * span_rows
        parts = tuple(
            (lax.dynamic_slice_in_dim(piece_part, offset, span_rows, 0) for piece_part in pieces)
        )
        group_qa, group_qb, group_pos, group_last = groups[0]

        def compute(inner, group_qa=group_qa, group_qb=group_qb, group_pos=group_pos):
            return (
                attend(inner[0], group_qa, parts[0], parts[1], offset, group_pos, DA),
                attend(inner[1], group_qb, parts[2], parts[3], offset, group_pos, DB),
            )

        updated = [lax.cond(offset <= group_last, compute, lambda inner: inner, carried[0])]
        return tuple(updated)

    final_state = lax.fori_loop(0, key_count // span_rows, one_span, initial)
    heads_out_a = finish(final_state[0][0], lambda_a, head_gain_a)
    heads_out_b = finish(final_state[0][1], lambda_b, head_gain_b)
    mixed_rows = lax.psum_scatter(
        (
            jnp.dot(heads_out_a, out_a, preferred_element_type=jnp.float32)
            + jnp.dot(heads_out_b, out_b, preferred_element_type=jnp.float32)
        ).astype(jnp.bfloat16),
        "tp",
        scatter_dimension=0,
        tiled=True,
    ).astype(jnp.float32)
    after_mix = (residual.astype(jnp.float32) + rms_norm(mixed_rows, gain_mix)).astype(jnp.bfloat16)
    normed = rms_norm(after_mix.astype(jnp.float32), gain_pre).astype(jnp.bfloat16)
    experts = lax.axis_size("sp")
    sub_rows = residual.shape[0]
    top_count = routes.shape[1]
    capacity = min(sub_rows, (5 * sub_rows * top_count + 4 * experts - 1) // (4 * experts))
    width = residual.shape[1]
    chips, tps = experts // CORES, lax.axis_size("tp")
    extra = -(-experts // 128) * 128
    shares = jnp.sum(
        jnp.where(
            routes[:, :, None] == jnp.arange(extra, dtype=jnp.int32)[None, None, :],
            route_weights[:, :, None],
            0.0,
        ),
        1,
    ).astype(jnp.bfloat16)
    gathered = gather_rows(jnp.concatenate([normed, shares], 1), chips, tps)
    parts = expert_parts(
        gathered, seq_slot, experts, capacity, width, (expert_gate[0], expert_up[0], expert_down[0])
    )
    routed = scatter_rows(parts, chips, tps)
    return (after_mix.astype(jnp.float32) + rms_norm(routed, gain_post)).astype(jnp.bfloat16)


def solution(mesh):
    in_specs = (
        P(("grp", "sp"), None, "tp"),
        P(("grp", "sp"), None, "tp"),
        P(("grp", "sp"), "tp"),
        P(("grp", "sp"), None, "tp"),
        P(("grp", "sp"), None, "tp"),
        P(("grp", "sp"), "tp"),
        P(),
        P(),
        P(),
        P("tp", None),
        P("tp", None),
        P(("grp", "sp", "tp"), None),
        P(),
        P(),
        P(),
        P(("grp", "sp", "tp"), None),
        P(("grp", "sp", "tp"), None),
        P("sp", None, "tp"),
        P("sp", None, "tp"),
        P("sp", "tp", None),
    )
    out_specs = P(("grp", "sp", "tp"), None)
    return jax.shard_map(
        per_device, mesh=mesh, in_specs=in_specs, out_specs=out_specs, check_vma=False
    )
```

```python
import jax
import jax.numpy as jnp
from jax import lax
from jax.experimental import pallas as pl
from jax.experimental.pallas import tpu as pltpu
from jax.sharding import PartitionSpec as P

HA = 4
DA = 128
DB = 64


def rms_norm(values, gain_vec):
    return values * lax.rsqrt(jnp.mean(values * values, -1, keepdims=True) + 1e-06) * gain_vec


MESH = pl.DeviceIdType.MESH
CORES = 2
LOG2E = 1.4426950408889634
VMEM_BYTES = 60 * 1024 * 1024


def place():
    sp = lax.axis_index("sp")
    return sp // CORES, sp % CORES, lax.axis_index("tp")


def greet(chips, tps):
    chip, core, tp = place()
    barrier = pltpu.get_barrier_semaphore()
    for step in range(1, chips):
        other = (chip + step) % chips
        pl.semaphore_signal(
            barrier, inc=1, device_id={"sp": other * CORES + core, "tp": tp}, device_id_type=MESH
        )
    for step in range(1, tps):
        pl.semaphore_signal(
            barrier,
            inc=1,
            device_id={"sp": chip * CORES + core, "tp": (tp + step) % tps},
            device_id_type=MESH,
        )
    pl.semaphore_signal(
        barrier, inc=1, device_id={"sp": chip * CORES + 1 - core, "tp": tp}, device_id_type=MESH
    )
    pl.semaphore_wait(barrier, chips - 1 + tps - 1 + 1)


def gather_kernel(chips, tps, own_ref, all_ref, send_sem, recv_sem, own_sem):
    chip, core, tp = place()
    greet(chips, tps)
    started = []

    def block(chip_of, core_of, tp_of):
        return (chip_of * CORES + core_of) * tps + tp_of

    def send(source, index, sp_to, tp_to):
        copy = pltpu.make_async_remote_copy(
            src_ref=source,
            dst_ref=all_ref.at[index],
            send_sem=send_sem.at[len(started)],
            recv_sem=recv_sem.at[index],
            device_id={"sp": sp_to, "tp": tp_to},
            device_id_type=MESH,
        )
        copy.start()
        started.append(copy)

    def arrived(index):
        pltpu.make_async_copy(all_ref.at[index], all_ref.at[index], recv_sem.at[index]).wait()

    own = block(chip, core, tp)
    for step in range(1, chips):
        send(own_ref, own, (chip + step) % chips * CORES + core, tp)
    for step in range(1, tps):
        send(own_ref, own, chip * CORES + core, (tp + step) % tps)
    send(own_ref, own, chip * CORES + 1 - core, tp)
    mine = pltpu.make_async_copy(own_ref, all_ref.at[own], own_sem)
    mine.start()

    def from_tp(chip_of):
        for step in range(1, tps):
            index = block(chip_of, core, (tp + step) % tps)
            arrived(index)
            send(all_ref.at[index], index, chip * CORES + 1 - core, tp)

    for step in range(1, chips):
        chip_of = (chip - step + chips) % chips
        index = block(chip_of, core, tp)
        arrived(index)
        for tp_step in range(1, tps):
            send(all_ref.at[index], index, chip * CORES + core, (tp + tp_step) % tps)
        send(all_ref.at[index], index, chip * CORES + 1 - core, tp)
        from_tp((chip - step + 1 + chips) % chips)
    from_tp((chip + 1) % chips)
    for step in range(chips):
        for tp_of in range(tps):
            arrived(block((chip - step + chips) % chips, 1 - core, (tp + tp_of) % tps))
    mine.wait()
    for copy in started:
        copy.wait_send()


def gather_rows(own, chips, tps):
    blocks = chips * CORES * tps
    sends = chips - 1 + tps - 1 + 1 + (chips - 1) * tps + chips * (tps - 1)
    return pl.pallas_call(
        lambda *refs: gather_kernel(chips, tps, *refs),
        name="gather_rows",
        out_shape=jax.ShapeDtypeStruct((blocks,) + own.shape, own.dtype),
        in_specs=[pl.BlockSpec(memory_space=pl.ANY)],
        out_specs=pl.BlockSpec(memory_space=pl.ANY),
        scratch_shapes=[
            pltpu.SemaphoreType.DMA((sends,)),
            pltpu.SemaphoreType.DMA((blocks,)),
            pltpu.SemaphoreType.DMA,
        ],
        compiler_params=pltpu.CompilerParams(collective_id=1, has_side_effects=True),
    )(own)


def add_rows(target, index, source, source_index):
    rows = target.shape[1]
    chunk = min(rows, 16)

    @pl.loop(0, rows // chunk)
    def _(part):
        span = pl.ds(pl.multiple_of(part * chunk, chunk), chunk)
        target[index, span, :] = (
            target[index, span, :].astype(jnp.float32)
            + source[source_index, span, :].astype(jnp.float32)
        ).astype(target.dtype)


def scatter_kernel(
    chips, tps, part_ref, out_ref, acc, core_in, tp_in, chip_in, load_sem, send_sem, core_sem, tp_sem, chip_sem
):
    chip, core, tp = place()
    load = []
    started = []
    for step in range(chips):
        for tp_step in range(tps):
            chip_of, tp_of = (chip + 1 + step) % chips, (tp + 1 + tp_step) % tps
            copy = pltpu.make_async_copy(
                part_ref.at[(chip_of * CORES + core) * tps + tp_of],
                acc.at[chip_of * tps + tp_of],
                load_sem.at[step * tps + tp_step],
            )
            copy.start()
            load.append(copy)
    greet(chips, tps)

    def send(source, target, recv_sem, sp_to, tp_to):
        copy = pltpu.make_async_remote_copy(
            src_ref=source,
            dst_ref=target,
            send_sem=send_sem.at[len(started)],
            recv_sem=recv_sem,
            device_id={"sp": sp_to, "tp": tp_to},
            device_id_type=MESH,
        )
        copy.start()
        started.append(copy)

    def arrived(target, index, sem):
        pltpu.make_async_copy(target.at[index], target.at[index], sem).wait()

    for step in range(chips):
        chip_of = (chip + 1 + step) % chips
        for tp_step in range(tps):
            tp_of = (tp + 1 + tp_step) % tps
            index = chip_of * tps + tp_of
            send(
                part_ref.at[(chip_of * CORES + 1 - core) * tps + tp_of],
                core_in.at[index],
                core_sem.at[index],
                chip * CORES + 1 - core,
                tp,
            )

    def chip_stage(step):
        chip_of = (chip + 1 + step) % chips
        for tp_step in range(1, tps):
            source = (tp + tp_step) % tps
            index = chip_of * tps + source
            arrived(tp_in, index, tp_sem.at[index])
            add_rows(acc, chip_of * tps + tp, tp_in, index)
        if step < chips - 1:
            send(
                acc.at[chip_of * tps + tp],
                chip_in.at[chip],
                chip_sem.at[chip],
                chip_of * CORES + core,
                tp,
            )

    for step in range(chips):
        chip_of = (chip + 1 + step) % chips
        for tp_step in range(tps):
            tp_of = (tp + 1 + tp_step) % tps
            index = chip_of * tps + tp_of
            load[step * tps + tp_step].wait()
            arrived(core_in, index, core_sem.at[index])
            add_rows(acc, index, core_in, index)
            if tp_step < tps - 1:
                send(
                    acc.at[index],
                    tp_in.at[chip_of * tps + tp],
                    tp_sem.at[chip_of * tps + tp],
                    chip * CORES + core,
                    tp_of,
                )
        if step > 0:
            chip_stage(step - 1)
    chip_stage(chips - 1)
    for step in range(1, chips):
        source = (chip - step + chips) % chips
        arrived(chip_in, source, chip_sem.at[source])
        if step < chips - 1:
            add_rows(acc, chip * tps + tp, chip_in, source)
    last = (chip + 1) % chips
    rows = out_ref.shape[0]
    chunk = min(rows, 16)

    @pl.loop(0, rows // chunk)
    def _(part):
        span = pl.ds(pl.multiple_of(part * chunk, chunk), chunk)
        out_ref[span, :] = acc[chip * tps + tp, span, :].astype(jnp.float32) + chip_in[
            last, span, :
        ].astype(jnp.float32)

    for copy in started:
        copy.wait_send()


def scatter_rows(parts, chips, tps):
    blocks, rows, width = parts.shape
    half = chips * tps
    sends = half + chips * (tps - 1) + chips - 1
    return pl.pallas_call(
        lambda *refs: scatter_kernel(chips, tps, *refs),
        name="scatter_rows",
        out_shape=jax.ShapeDtypeStruct((rows, width), jnp.float32),
        in_specs=[pl.BlockSpec(memory_space=pl.ANY)],
        out_specs=pl.BlockSpec(memory_space=pltpu.VMEM),
        scratch_shapes=[
            pltpu.VMEM((half, rows, width), parts.dtype),
            pltpu.VMEM((half, rows, width), parts.dtype),
            pltpu.VMEM((half, rows, width), parts.dtype),
            pltpu.VMEM((chips, rows, width), parts.dtype),
            pltpu.SemaphoreType.DMA((half,)),
            pltpu.SemaphoreType.DMA((sends,)),
            pltpu.SemaphoreType.DMA((half,)),
            pltpu.SemaphoreType.DMA((half,)),
            pltpu.SemaphoreType.DMA((chips,)),
        ],
        compiler_params=pltpu.CompilerParams(
            collective_id=2, has_side_effects=True, vmem_limit_bytes=VMEM_BYTES
        ),
    )(parts)


def attend_kernel(
    chips, heads_a, heads_b, query_ref, own_ref, lambda_ref, gain_a_ref, gain_b_ref, out_ref,
    held, top, total, accum_a, accum_b, own_sem, up_sem, side_sem, recv_sem,
):
    chip, core, tp = place()
    me = chip * CORES + core
    rows = own_ref.shape[0]
    mine = pltpu.make_async_copy(own_ref, held.at[me], own_sem)
    mine.start()
    barrier = pltpu.get_barrier_semaphore()

    def hello(sp_to):
        pl.semaphore_signal(barrier, inc=1, device_id={"sp": sp_to, "tp": tp}, device_id_type=MESH)

    hello(chip * CORES + 1 - core)

    @pl.when(chip > 0)
    def _():
        hello(me - CORES)

    @pl.when(chip < chips - 1)
    def _():
        hello(me + CORES)

    pl.semaphore_wait(
        barrier, 1 + jnp.where(chip > 0, 1, 0) + jnp.where(chip < chips - 1, 1, 0)
    )

    top[...] = jnp.full_like(top, -1e30)
    total[...] = jnp.zeros_like(total)
    accum_a[...] = jnp.zeros_like(accum_a)
    accum_b[...] = jnp.zeros_like(accum_b)
    mine.wait()

    def copy_up(back, index):
        return pltpu.make_async_remote_copy(
            src_ref=held.at[index], dst_ref=held.at[index], send_sem=up_sem.at[back],
            recv_sem=recv_sem.at[index], device_id={"sp": me + CORES, "tp": tp}, device_id_type=MESH,
        )

    def copy_side(back, index):
        return pltpu.make_async_remote_copy(
            src_ref=held.at[index], dst_ref=held.at[index], send_sem=side_sem.at[back],
            recv_sem=recv_sem.at[index], device_id={"sp": chip * CORES + 1 - core, "tp": tp},
            device_id_type=MESH,
        )

    base_va = 2 * heads_a * DA
    base_kb = base_va + heads_a * 2 * DA
    base_vb = base_kb + 2 * heads_b * DB
    base_qb = 2 * heads_a * DA
    ahead = lax.broadcasted_iota(jnp.int32, (rows, rows), 0) - lax.broadcasted_iota(
        jnp.int32, (rows, rows), 1
    )

    def flash(index):
        shown = ahead + (me - index) * rows >= 0

        def one(slot, query, key, value, accum, part, size):
            scores = lax.dot_general(
                query, key, (((1,), (1,)), ((), ())), preferred_element_type=jnp.float32
            )
            scores = jnp.where(shown, scores, -1e30)
            before = top[slot]
            after = jnp.maximum(before, jnp.max(scores, -1, keepdims=True))
            factor = size ** (-0.5) * LOG2E
            terms = jnp.exp2((scores - after) * factor)
            rescale = jnp.exp2((before - after) * factor)
            top[slot] = after
            total[slot] = total[slot] * rescale + jnp.sum(terms, -1, keepdims=True)
            accum[part] = accum[part] * rescale + jnp.dot(
                terms.astype(jnp.bfloat16), value, preferred_element_type=jnp.float32
            )

        for head in range(heads_a):
            value = held[index, :, base_va + head * 2 * DA : base_va + (head + 1) * 2 * DA]
            for pair in range(2):
                at = (pair * heads_a + head) * DA
                part = pair * heads_a + head
                one(
                    part, query_ref[:, at : at + DA], held[index, :, at : at + DA], value,
                    accum_a, part, DA,
                )
        for head in range(heads_b):
            value = held[index, :, base_vb + head * 2 * DB : base_vb + (head + 1) * 2 * DB]
            for pair in range(2):
                part = pair * heads_b + head
                at = base_qb + part * 2 * DB
                key_at = base_kb + part // 2 * 2 * DB
                one(
                    2 * heads_a + part, query_ref[:, at : at + 2 * DB],
                    held[index, :, key_at : key_at + 2 * DB], value, accum_b, part, DB,
                )

    def step(number, carry):
        back = number // 2
        side = number % 2
        source = chip - back

        @pl.when(source >= 0)
        def _():
            index = source * CORES + jnp.where(side == 0, core, 1 - core)

            @pl.when(number > 0)
            def _():
                pltpu.make_async_copy(held.at[index], held.at[index], recv_sem.at[index]).wait()

            @pl.when(side == 0)
            def _():
                @pl.when(chip < chips - 1)
                def _():
                    copy_up(back, index).start()

                copy_side(back, index).start()

            @pl.when(index <= me)
            def _():
                flash(index)

        return carry

    lax.fori_loop(0, 2 * chips, step, 0)

    def finish(head, parts, accum, slots, lam, gain_ref, at, wide):
        mixture = accum[parts[0]] / total[slots[0]] - lam * accum[parts[1]] / total[slots[1]]
        out_ref[:, at : at + wide] = rms_norm(mixture, gain_ref[...]).astype(out_ref.dtype)

    for head in range(heads_a):
        parts = (head, heads_a + head)
        finish(head, parts, accum_a, parts, lambda_ref[0:1, head : head + 1], gain_a_ref,
               head * 2 * DA, 2 * DA)
    for head in range(heads_b):
        parts = (head, heads_b + head)
        slots = (2 * heads_a + head, 2 * heads_a + heads_b + head)
        finish(head, parts, accum_b, slots, lambda_ref[0:1, heads_a + head : heads_a + head + 1],
               gain_b_ref, heads_a * 2 * DA + head * 2 * DB, 2 * DB)

    def settle(back, carry):
        @pl.when(chip - back >= 0)
        def _():
            index = (chip - back) * CORES + core

            @pl.when(chip < chips - 1)
            def _():
                copy_up(back, index).wait_send()

            copy_side(back, index).wait_send()

        return carry

    lax.fori_loop(0, chips, settle, 0)


def attend_blocks(queries, own, lambdas, gain_a, gain_b, chips, heads_a, heads_b):
    rows, width = own.shape
    vmem = pl.BlockSpec(memory_space=pltpu.VMEM)
    return pl.pallas_call(
        lambda *refs: attend_kernel(chips, heads_a, heads_b, *refs),
        name="attend_blocks",
        out_shape=jax.ShapeDtypeStruct((rows, heads_a * 2 * DA + heads_b * 2 * DB), jnp.bfloat16),
        in_specs=[vmem, pl.BlockSpec(memory_space=pl.ANY), vmem, vmem, vmem],
        out_specs=vmem,
        scratch_shapes=[
            pltpu.VMEM((chips * CORES, rows, width), own.dtype),
            pltpu.VMEM((2 * (heads_a + heads_b), rows, 1), jnp.float32),
            pltpu.VMEM((2 * (heads_a + heads_b), rows, 1), jnp.float32),
            pltpu.VMEM((2 * heads_a, rows, 2 * DA), jnp.float32),
            pltpu.VMEM((2 * heads_b, rows, 2 * DB), jnp.float32),
            pltpu.SemaphoreType.DMA,
            pltpu.SemaphoreType.DMA((chips,)),
            pltpu.SemaphoreType.DMA((chips,)),
            pltpu.SemaphoreType.DMA((chips * CORES,)),
        ],
        compiler_params=pltpu.CompilerParams(
            collective_id=3, has_side_effects=True, vmem_limit_bytes=VMEM_BYTES
        ),
    )(queries, own, lambdas, gain_a, gain_b)


def share_kernel(tps, part_ref, out_ref, arrived, send_sem, recv_sem):
    tp = lax.axis_index("tp")
    barrier = pltpu.get_barrier_semaphore()
    for step in range(1, tps):
        pl.semaphore_signal(barrier, inc=1, device_id={"tp": (tp + step) % tps}, device_id_type=MESH)
    pl.semaphore_wait(barrier, tps - 1)
    started = []
    for step in range(1, tps):
        other = (tp + step) % tps
        copy = pltpu.make_async_remote_copy(
            src_ref=part_ref.at[other], dst_ref=arrived.at[step - 1], send_sem=send_sem.at[step - 1],
            recv_sem=recv_sem.at[step - 1], device_id={"tp": other}, device_id_type=MESH,
        )
        copy.start()
        started.append(copy)
    rows = out_ref.shape[0]
    chunk = min(rows, 16)
    for step in range(1, tps):
        started[step - 1].wait()

        @pl.loop(0, rows // chunk)
        def _(part):
            span = pl.ds(pl.multiple_of(part * chunk, chunk), chunk)
            first = part_ref[tp, span, :].astype(jnp.float32) if step == 1 else out_ref[span, :]
            out_ref[span, :] = first + arrived[step - 1, span, :].astype(jnp.float32)


def share_rows(parts, tps):
    _, rows, width = parts.shape
    vmem = pl.BlockSpec(memory_space=pltpu.VMEM)
    return pl.pallas_call(
        lambda *refs: share_kernel(tps, *refs),
        name="share_rows",
        out_shape=jax.ShapeDtypeStruct((rows, width), jnp.float32),
        in_specs=[vmem],
        out_specs=vmem,
        scratch_shapes=[
            pltpu.VMEM((tps - 1, rows, width), parts.dtype),
            pltpu.SemaphoreType.DMA((tps - 1,)),
            pltpu.SemaphoreType.DMA((tps - 1,)),
        ],
        compiler_params=pltpu.CompilerParams(collective_id=4, has_side_effects=True),
    )(parts)


def spread_pairs(queries, heads):
    rows = queries.shape[0]
    pairs = queries.reshape(rows, 2 * heads // 2, 1, 2, DB)
    keep = jnp.eye(2, dtype=queries.dtype).reshape(1, 1, 2, 2, 1)
    return (pairs * keep).reshape(rows, 2 * heads * 2 * DB)


def expert_parts(gathered, expert, experts, capacity, width, weights):
    gate, up, down = weights
    blocks, rows, _ = gathered.shape
    shares = lax.dynamic_slice_in_dim(gathered[:, :, width:], expert, 1, 2)[:, :, 0]
    named = shares > 0
    order = jnp.arange(rows, dtype=jnp.int32)
    slots = jnp.dot(
        named.astype(jnp.bfloat16),
        (order[:, None] < order[None, :]).astype(jnp.bfloat16),
        preferred_element_type=jnp.float32,
    ).astype(jnp.int32)
    picks = (slots[:, None, :] == jnp.arange(capacity, dtype=jnp.int32)[None, :, None]) & named[:, None, :]
    rows_in = jnp.einsum(
        "bct,btd->bcd",
        picks.astype(jnp.bfloat16),
        gathered[:, :, :width],
        preferred_element_type=jnp.float32,
    ).astype(jnp.bfloat16)
    rows_in = rows_in.reshape(blocks * capacity, width)
    gate_pre = jnp.dot(rows_in, gate, preferred_element_type=jnp.float32)
    up_pre = jnp.dot(rows_in, up, preferred_element_type=jnp.float32)
    glu_part = jnp.minimum(gate_pre, 7.0)
    lin_part = jnp.clip(up_pre, -7.0, 7.0)
    hidden = (glu_part * jax.nn.sigmoid(1.702 * glu_part) * (lin_part + 1.0)).astype(jnp.bfloat16)
    outs = jnp.dot(hidden, down, preferred_element_type=jnp.float32).astype(jnp.bfloat16)
    back = jnp.where(picks, shares[:, None, :], 0).astype(jnp.bfloat16)
    return jnp.einsum(
        "bct,bcd->btd",
        back,
        outs.reshape(blocks, capacity, width),
        preferred_element_type=jnp.float32,
    ).astype(jnp.bfloat16)


def per_device(
    queries_a,
    keys_a,
    values_a,
    queries_b,
    keys_b,
    values_b,
    lambdas,
    head_gain_a,
    head_gain_b,
    out_a,
    out_b,
    residual,
    gain_mix,
    gain_pre,
    gain_post,
    routes,
    route_weights,
    expert_gate,
    expert_up,
    expert_down,
):
    length = queries_a.shape[0]
    heads_a = queries_a.shape[2] // DA
    heads_b = queries_b.shape[2] // DB
    head_slot = lax.axis_index("tp")
    seq_slot = lax.axis_index("sp")
    lambda_a = lax.dynamic_slice_in_dim(lambdas, head_slot * heads_a, heads_a)
    lambda_b = lax.dynamic_slice_in_dim(lambdas, HA + head_slot * heads_b, heads_b)
    experts, tps = lax.axis_size("sp"), lax.axis_size("tp")
    chips = experts // CORES
    own = jnp.concatenate(
        [keys_a.reshape(length, -1), values_a, keys_b.reshape(length, -1), values_b], 1
    )
    queries = jnp.concatenate([queries_a.reshape(length, -1), spread_pairs(queries_b, heads_b)], 1)
    heads_out = attend_blocks(
        queries,
        own,
        jnp.concatenate([lambda_a, lambda_b])[None],
        head_gain_a[None],
        head_gain_b[None],
        chips,
        heads_a,
        heads_b,
    )
    cut = heads_a * 2 * DA
    mixed = (
        jnp.dot(heads_out[:, :cut], out_a, preferred_element_type=jnp.float32)
        + jnp.dot(heads_out[:, cut:], out_b, preferred_element_type=jnp.float32)
    ).astype(jnp.bfloat16)
    mixed_rows = share_rows(mixed.reshape(tps, length // tps, -1), tps)
    after_mix = (residual.astype(jnp.float32) + rms_norm(mixed_rows, gain_mix)).astype(jnp.bfloat16)
    normed = rms_norm(after_mix.astype(jnp.float32), gain_pre).astype(jnp.bfloat16)
    sub_rows = residual.shape[0]
    top_count = routes.shape[1]
    capacity = min(sub_rows, (5 * sub_rows * top_count + 4 * experts - 1) // (4 * experts))
    width = residual.shape[1]
    extra = -(-experts // 128) * 128
    shares = jnp.sum(
        jnp.where(
            routes[:, :, None] == jnp.arange(extra, dtype=jnp.int32)[None, None, :],
            route_weights[:, :, None],
            0.0,
        ),
        1,
    ).astype(jnp.bfloat16)
    gathered = gather_rows(jnp.concatenate([normed, shares], 1), chips, tps)
    parts = expert_parts(
        gathered, seq_slot, experts, capacity, width, (expert_gate[0], expert_up[0], expert_down[0])
    )
    routed = scatter_rows(parts, chips, tps)
    return (after_mix.astype(jnp.float32) + rms_norm(routed, gain_post)).astype(jnp.bfloat16)


def solution(mesh):
    in_specs = (
        P(("grp", "sp"), None, "tp"),
        P(("grp", "sp"), None, "tp"),
        P(("grp", "sp"), "tp"),
        P(("grp", "sp"), None, "tp"),
        P(("grp", "sp"), None, "tp"),
        P(("grp", "sp"), "tp"),
        P(),
        P(),
        P(),
        P("tp", None),
        P("tp", None),
        P(("grp", "sp", "tp"), None),
        P(),
        P(),
        P(),
        P(("grp", "sp", "tp"), None),
        P(("grp", "sp", "tp"), None),
        P("sp", None, "tp"),
        P("sp", None, "tp"),
        P("sp", "tp", None),
    )
    out_specs = P(("grp", "sp", "tp"), None)
    return jax.shard_map(
        per_device, mesh=mesh, in_specs=in_specs, out_specs=out_specs, check_vma=False
    )
```

```python
import jax
import jax.numpy as jnp
from jax import lax
from jax.experimental import pallas as pl
from jax.experimental.pallas import tpu as pltpu
from jax.sharding import PartitionSpec as P

HA = 4
DA = 128
DB = 64


def rms_norm(values, gain_vec):
    return values * lax.rsqrt(jnp.mean(values * values, -1, keepdims=True) + 1e-06) * gain_vec


MESH = pl.DeviceIdType.MESH
CORES = 2
PIECES = 2
LOG2E = 1.4426950408889634
VMEM_BYTES = 60 * 1024 * 1024


def place():
    sp = lax.axis_index("sp")
    return sp // CORES, sp % CORES, lax.axis_index("tp")


def greet(chips, tps):
    chip, core, tp = place()
    barrier = pltpu.get_barrier_semaphore()
    for step in range(1, chips):
        other = (chip + step) % chips
        pl.semaphore_signal(
            barrier, inc=1, device_id={"sp": other * CORES + core, "tp": tp}, device_id_type=MESH
        )
    for step in range(1, tps):
        pl.semaphore_signal(
            barrier,
            inc=1,
            device_id={"sp": chip * CORES + core, "tp": (tp + step) % tps},
            device_id_type=MESH,
        )
    pl.semaphore_signal(
        barrier, inc=1, device_id={"sp": chip * CORES + 1 - core, "tp": tp}, device_id_type=MESH
    )
    pl.semaphore_wait(barrier, chips - 1 + tps - 1 + 1)


def gather_kernel(chips, tps, own_ref, all_ref, send_sem, recv_sem, own_sem):
    chip, core, tp = place()
    greet(chips, tps)
    started = []

    def block(chip_of, core_of, tp_of, piece):
        return ((chip_of * CORES + core_of) * tps + tp_of) * PIECES + piece

    def send(source, index, sp_to, tp_to):
        copy = pltpu.make_async_remote_copy(
            src_ref=source,
            dst_ref=all_ref.at[index],
            send_sem=send_sem.at[len(started)],
            recv_sem=recv_sem.at[index],
            device_id={"sp": sp_to, "tp": tp_to},
            device_id_type=MESH,
        )
        copy.start()
        started.append(copy)

    def arrived(index):
        pltpu.make_async_copy(all_ref.at[index], all_ref.at[index], recv_sem.at[index]).wait()

    for piece in range(PIECES):
        own = block(chip, core, tp, piece)
        for step in range(1, tps):
            send(own_ref.at[piece], own, chip * CORES + core, (tp + step) % tps)
        for step in range(1, chips):
            send(own_ref.at[piece], own, (chip + step) % chips * CORES + core, tp)
        send(own_ref.at[piece], own, chip * CORES + 1 - core, tp)
    mine = pltpu.make_async_copy(
        own_ref, all_ref.at[pl.ds(block(chip, core, tp, 0), PIECES)], own_sem
    )
    mine.start()

    def from_tp(chip_of, piece):
        for step in range(1, tps):
            index = block(chip_of, core, (tp + step) % tps, piece)
            arrived(index)
            send(all_ref.at[index], index, chip * CORES + 1 - core, tp)

    order = [(step, piece) for step in range(chips) for piece in range(PIECES)]
    for place_in, (step, piece) in enumerate(order):
        if step > 0:
            index = block((chip - step + chips) % chips, core, tp, piece)
            arrived(index)
            for tp_step in range(1, tps):
                send(all_ref.at[index], index, chip * CORES + core, (tp + tp_step) % tps)
            send(all_ref.at[index], index, chip * CORES + 1 - core, tp)
            done, done_piece = order[place_in - PIECES]
            from_tp((chip - done + chips) % chips, done_piece)
    for piece in range(PIECES):
        from_tp((chip + 1) % chips, piece)
    for step, piece in order:
        for tp_of in range(tps):
            arrived(block((chip - step + chips) % chips, 1 - core, (tp + tp_of) % tps, piece))
    mine.wait()
    for copy in started:
        copy.wait_send()


def gather_rows(own, chips, tps):
    blocks = chips * CORES * tps * PIECES
    sends = (chips - 1 + tps - 1 + 1 + (chips - 1) * tps + chips * (tps - 1)) * PIECES
    rows, width = own.shape
    own = own.reshape(PIECES, rows // PIECES, width)
    return pl.pallas_call(
        lambda *refs: gather_kernel(chips, tps, *refs),
        name="gather_rows",
        out_shape=jax.ShapeDtypeStruct((blocks,) + own.shape[1:], own.dtype),
        in_specs=[pl.BlockSpec(memory_space=pl.ANY)],
        out_specs=pl.BlockSpec(memory_space=pl.ANY),
        scratch_shapes=[
            pltpu.SemaphoreType.DMA((sends,)),
            pltpu.SemaphoreType.DMA((blocks,)),
            pltpu.SemaphoreType.DMA,
        ],
        compiler_params=pltpu.CompilerParams(collective_id=1, has_side_effects=True),
    )(own).reshape(-1, rows, width)


def add_rows(target, index, source, source_index):
    rows = target.shape[1]
    chunk = min(rows, 16)

    @pl.loop(0, rows // chunk)
    def _(part):
        span = pl.ds(pl.multiple_of(part * chunk, chunk), chunk)
        target[index, span, :] = (
            target[index, span, :].astype(jnp.float32)
            + source[source_index, span, :].astype(jnp.float32)
        ).astype(target.dtype)


def scatter_kernel(
    chips, tps, part_ref, out_ref, acc, core_in, tp_in, chip_in, load_sem, send_sem, core_sem, tp_sem, chip_sem
):
    chip, core, tp = place()
    load = []
    started = []
    order = [(step, piece) for step in range(chips) for piece in range(PIECES)]
    for step, piece in order:
        for tp_step in range(tps):
            chip_of, tp_of = (chip + 1 + step) % chips, (tp + 1 + tp_step) % tps
            copy = pltpu.make_async_copy(
                part_ref.at[((chip_of * CORES + core) * tps + tp_of) * PIECES + piece],
                acc.at[(chip_of * tps + tp_of) * PIECES + piece],
                load_sem.at[len(load)],
            )
            copy.start()
            load.append(copy)
    greet(chips, tps)

    def send(source, target, recv_sem, sp_to, tp_to):
        copy = pltpu.make_async_remote_copy(
            src_ref=source,
            dst_ref=target,
            send_sem=send_sem.at[len(started)],
            recv_sem=recv_sem,
            device_id={"sp": sp_to, "tp": tp_to},
            device_id_type=MESH,
        )
        copy.start()
        started.append(copy)

    def arrived(target, index, sem):
        pltpu.make_async_copy(target.at[index], target.at[index], sem).wait()

    for step, piece in order:
        chip_of = (chip + 1 + step) % chips
        for tp_step in range(tps):
            tp_of = (tp + 1 + tp_step) % tps
            index = (chip_of * tps + tp_of) * PIECES + piece
            send(
                part_ref.at[((chip_of * CORES + 1 - core) * tps + tp_of) * PIECES + piece],
                core_in.at[index],
                core_sem.at[index],
                chip * CORES + 1 - core,
                tp,
            )

    def chip_stage(step, piece):
        chip_of = (chip + 1 + step) % chips
        kept = (chip_of * tps + tp) * PIECES + piece
        for tp_step in range(1, tps):
            index = (chip_of * tps + (tp + tp_step) % tps) * PIECES + piece
            arrived(tp_in, index, tp_sem.at[index])
            add_rows(acc, kept, tp_in, index)
        if step < chips - 1:
            slot = chip * PIECES + piece
            send(acc.at[kept], chip_in.at[slot], chip_sem.at[slot], chip_of * CORES + core, tp)

    for number, (step, piece) in enumerate(order):
        chip_of = (chip + 1 + step) % chips
        for tp_step in range(tps):
            tp_of = (tp + 1 + tp_step) % tps
            index = (chip_of * tps + tp_of) * PIECES + piece
            load[number * tps + tp_step].wait()
            arrived(core_in, index, core_sem.at[index])
            add_rows(acc, index, core_in, index)
            if tp_step < tps - 1:
                slot = (chip_of * tps + tp) * PIECES + piece
                send(
                    acc.at[index], tp_in.at[slot], tp_sem.at[slot], chip * CORES + core, tp_of
                )
        if number > 0:
            chip_stage(*order[number - 1])
    chip_stage(*order[-1])
    rows = out_ref.shape[1]
    chunk = min(rows, 16)
    for step in range(1, chips):
        for piece in range(PIECES):
            source = (chip - step + chips) % chips * PIECES + piece
            kept = (chip * tps + tp) * PIECES + piece
            arrived(chip_in, source, chip_sem.at[source])
            if step < chips - 1:
                add_rows(acc, kept, chip_in, source)
            else:

                @pl.loop(0, rows // chunk)
                def _(part):
                    span = pl.ds(pl.multiple_of(part * chunk, chunk), chunk)
                    out_ref[piece, span, :] = acc[kept, span, :].astype(jnp.float32) + chip_in[
                        source, span, :
                    ].astype(jnp.float32)

    for copy in started:
        copy.wait_send()


def scatter_rows(parts, chips, tps):
    blocks, rows, width = parts.shape
    half = chips * tps * PIECES
    sends = half + (chips * (tps - 1) + chips - 1) * PIECES
    rows = rows // PIECES
    return pl.pallas_call(
        lambda *refs: scatter_kernel(chips, tps, *refs),
        name="scatter_rows",
        out_shape=jax.ShapeDtypeStruct((PIECES, rows, width), jnp.float32),
        in_specs=[pl.BlockSpec(memory_space=pl.ANY)],
        out_specs=pl.BlockSpec(memory_space=pltpu.VMEM),
        scratch_shapes=[
            pltpu.VMEM((half, rows, width), parts.dtype),
            pltpu.VMEM((half, rows, width), parts.dtype),
            pltpu.VMEM((half, rows, width), parts.dtype),
            pltpu.VMEM((chips * PIECES, rows, width), parts.dtype),
            pltpu.SemaphoreType.DMA((half,)),
            pltpu.SemaphoreType.DMA((sends,)),
            pltpu.SemaphoreType.DMA((half,)),
            pltpu.SemaphoreType.DMA((half,)),
            pltpu.SemaphoreType.DMA((chips * PIECES,)),
        ],
        compiler_params=pltpu.CompilerParams(
            collective_id=2, has_side_effects=True, vmem_limit_bytes=VMEM_BYTES
        ),
    )(parts.reshape(-1, rows, width)).reshape(PIECES * rows, width)


def attend_kernel(
    chips, heads_a, heads_b, query_ref, own_ref, lambda_ref, gain_a_ref, gain_b_ref, out_ref,
    held, top, total, accum_a, accum_b, own_sem, up_sem, side_sem, recv_sem,
):
    chip, core, tp = place()
    me = chip * CORES + core
    rows = own_ref.shape[0]
    mine = pltpu.make_async_copy(own_ref, held.at[me], own_sem)
    mine.start()
    barrier = pltpu.get_barrier_semaphore()

    def hello(sp_to):
        pl.semaphore_signal(barrier, inc=1, device_id={"sp": sp_to, "tp": tp}, device_id_type=MESH)

    hello(chip * CORES + 1 - core)

    @pl.when(chip > 0)
    def _():
        hello(me - CORES)

    @pl.when(chip < chips - 1)
    def _():
        hello(me + CORES)

    pl.semaphore_wait(
        barrier, 1 + jnp.where(chip > 0, 1, 0) + jnp.where(chip < chips - 1, 1, 0)
    )

    top[...] = jnp.full_like(top, -1e30)
    total[...] = jnp.zeros_like(total)
    accum_a[...] = jnp.zeros_like(accum_a)
    accum_b[...] = jnp.zeros_like(accum_b)
    mine.wait()

    def copy_up(back, index):
        return pltpu.make_async_remote_copy(
            src_ref=held.at[index], dst_ref=held.at[index], send_sem=up_sem.at[back],
            recv_sem=recv_sem.at[index], device_id={"sp": me + CORES, "tp": tp}, device_id_type=MESH,
        )

    def copy_side(back, index):
        return pltpu.make_async_remote_copy(
            src_ref=held.at[index], dst_ref=held.at[index], send_sem=side_sem.at[back],
            recv_sem=recv_sem.at[index], device_id={"sp": chip * CORES + 1 - core, "tp": tp},
            device_id_type=MESH,
        )

    base_va = 2 * heads_a * DA
    base_kb = base_va + heads_a * 2 * DA
    base_vb = base_kb + 2 * heads_b * DB
    base_qb = 2 * heads_a * DA
    ahead = lax.broadcasted_iota(jnp.int32, (rows, rows), 0) - lax.broadcasted_iota(
        jnp.int32, (rows, rows), 1
    )

    def flash(index):
        shown = ahead + (me - index) * rows >= 0

        def one(slot, query, key, value, accum, part, size):
            scores = lax.dot_general(
                query, key, (((1,), (1,)), ((), ())), preferred_element_type=jnp.float32
            )
            scores = jnp.where(shown, scores, -1e30)
            before = top[slot]
            after = jnp.maximum(before, jnp.max(scores, -1, keepdims=True))
            factor = size ** (-0.5) * LOG2E
            terms = jnp.exp2((scores - after) * factor)
            rescale = jnp.exp2((before - after) * factor)
            top[slot] = after
            total[slot] = total[slot] * rescale + jnp.sum(terms, -1, keepdims=True)
            accum[part] = accum[part] * rescale + jnp.dot(
                terms.astype(jnp.bfloat16), value, preferred_element_type=jnp.float32
            )

        for head in range(heads_a):
            value = held[index, :, base_va + head * 2 * DA : base_va + (head + 1) * 2 * DA]
            for pair in range(2):
                at = (pair * heads_a + head) * DA
                part = pair * heads_a + head
                one(
                    part, query_ref[:, at : at + DA], held[index, :, at : at + DA], value,
                    accum_a, part, DA,
                )
        for head in range(heads_b):
            value = held[index, :, base_vb + head * 2 * DB : base_vb + (head + 1) * 2 * DB]
            for pair in range(2):
                part = pair * heads_b + head
                at = base_qb + part * 2 * DB
                key_at = base_kb + part // 2 * 2 * DB
                one(
                    2 * heads_a + part, query_ref[:, at : at + 2 * DB],
                    held[index, :, key_at : key_at + 2 * DB], value, accum_b, part, DB,
                )

    def step(number, carry):
        back = number // 2
        side = number % 2
        source = chip - back

        @pl.when(source >= 0)
        def _():
            index = source * CORES + jnp.where(side == 0, core, 1 - core)

            @pl.when(number > 0)
            def _():
                pltpu.make_async_copy(held.at[index], held.at[index], recv_sem.at[index]).wait()

            @pl.when(side == 0)
            def _():
                @pl.when(chip < chips - 1)
                def _():
                    copy_up(back, index).start()

                copy_side(back, index).start()

            @pl.when(index <= me)
            def _():
                flash(index)

        return carry

    lax.fori_loop(0, 2 * chips, step, 0)

    def finish(head, parts, accum, slots, lam, gain_ref, at, wide):
        mixture = accum[parts[0]] / total[slots[0]] - lam * accum[parts[1]] / total[slots[1]]
        out_ref[:, at : at + wide] = rms_norm(mixture, gain_ref[...]).astype(out_ref.dtype)

    for head in range(heads_a):
        parts = (head, heads_a + head)
        finish(head, parts, accum_a, parts, lambda_ref[0:1, head : head + 1], gain_a_ref,
               head * 2 * DA, 2 * DA)
    for head in range(heads_b):
        parts = (head, heads_b + head)
        slots = (2 * heads_a + head, 2 * heads_a + heads_b + head)
        finish(head, parts, accum_b, slots, lambda_ref[0:1, heads_a + head : heads_a + head + 1],
               gain_b_ref, heads_a * 2 * DA + head * 2 * DB, 2 * DB)

    def settle(back, carry):
        @pl.when(chip - back >= 0)
        def _():
            index = (chip - back) * CORES + core

            @pl.when(chip < chips - 1)
            def _():
                copy_up(back, index).wait_send()

            copy_side(back, index).wait_send()

        return carry

    lax.fori_loop(0, chips, settle, 0)


def attend_blocks(queries, own, lambdas, gain_a, gain_b, chips, heads_a, heads_b):
    rows, width = own.shape
    vmem = pl.BlockSpec(memory_space=pltpu.VMEM)
    return pl.pallas_call(
        lambda *refs: attend_kernel(chips, heads_a, heads_b, *refs),
        name="attend_blocks",
        out_shape=jax.ShapeDtypeStruct((rows, heads_a * 2 * DA + heads_b * 2 * DB), jnp.bfloat16),
        in_specs=[vmem, pl.BlockSpec(memory_space=pl.ANY), vmem, vmem, vmem],
        out_specs=vmem,
        scratch_shapes=[
            pltpu.VMEM((chips * CORES, rows, width), own.dtype),
            pltpu.VMEM((2 * (heads_a + heads_b), rows, 1), jnp.float32),
            pltpu.VMEM((2 * (heads_a + heads_b), rows, 1), jnp.float32),
            pltpu.VMEM((2 * heads_a, rows, 2 * DA), jnp.float32),
            pltpu.VMEM((2 * heads_b, rows, 2 * DB), jnp.float32),
            pltpu.SemaphoreType.DMA,
            pltpu.SemaphoreType.DMA((chips,)),
            pltpu.SemaphoreType.DMA((chips,)),
            pltpu.SemaphoreType.DMA((chips * CORES,)),
        ],
        compiler_params=pltpu.CompilerParams(
            collective_id=3, has_side_effects=True, vmem_limit_bytes=VMEM_BYTES
        ),
    )(queries, own, lambdas, gain_a, gain_b)


def share_kernel(tps, part_ref, out_ref, arrived, send_sem, recv_sem):
    tp = lax.axis_index("tp")
    barrier = pltpu.get_barrier_semaphore()
    for step in range(1, tps):
        pl.semaphore_signal(barrier, inc=1, device_id={"tp": (tp + step) % tps}, device_id_type=MESH)
    pl.semaphore_wait(barrier, tps - 1)
    started = []
    for step in range(1, tps):
        other = (tp + step) % tps
        copy = pltpu.make_async_remote_copy(
            src_ref=part_ref.at[other], dst_ref=arrived.at[step - 1], send_sem=send_sem.at[step - 1],
            recv_sem=recv_sem.at[step - 1], device_id={"tp": other}, device_id_type=MESH,
        )
        copy.start()
        started.append(copy)
    rows = out_ref.shape[0]
    chunk = min(rows, 16)
    for step in range(1, tps):
        started[step - 1].wait()

        @pl.loop(0, rows // chunk)
        def _(part):
            span = pl.ds(pl.multiple_of(part * chunk, chunk), chunk)
            first = part_ref[tp, span, :].astype(jnp.float32) if step == 1 else out_ref[span, :]
            out_ref[span, :] = first + arrived[step - 1, span, :].astype(jnp.float32)


def share_rows(parts, tps):
    _, rows, width = parts.shape
    vmem = pl.BlockSpec(memory_space=pltpu.VMEM)
    return pl.pallas_call(
        lambda *refs: share_kernel(tps, *refs),
        name="share_rows",
        out_shape=jax.ShapeDtypeStruct((rows, width), jnp.float32),
        in_specs=[vmem],
        out_specs=vmem,
        scratch_shapes=[
            pltpu.VMEM((tps - 1, rows, width), parts.dtype),
            pltpu.SemaphoreType.DMA((tps - 1,)),
            pltpu.SemaphoreType.DMA((tps - 1,)),
        ],
        compiler_params=pltpu.CompilerParams(collective_id=4, has_side_effects=True),
    )(parts)


def spread_pairs(queries, heads):
    rows = queries.shape[0]
    pairs = queries.reshape(rows, 2 * heads // 2, 1, 2, DB)
    keep = jnp.eye(2, dtype=queries.dtype).reshape(1, 1, 2, 2, 1)
    return (pairs * keep).reshape(rows, 2 * heads * 2 * DB)


def expert_parts(gathered, expert, experts, capacity, width, weights):
    gate, up, down = weights
    blocks, rows, _ = gathered.shape
    shares = lax.dynamic_slice_in_dim(gathered[:, :, width:], expert, 1, 2)[:, :, 0]
    named = shares > 0
    order = jnp.arange(rows, dtype=jnp.int32)
    slots = jnp.dot(
        named.astype(jnp.bfloat16),
        (order[:, None] < order[None, :]).astype(jnp.bfloat16),
        preferred_element_type=jnp.float32,
    ).astype(jnp.int32)
    picks = (slots[:, None, :] == jnp.arange(capacity, dtype=jnp.int32)[None, :, None]) & named[:, None, :]
    rows_in = jnp.einsum(
        "bct,btd->bcd",
        picks.astype(jnp.bfloat16),
        gathered[:, :, :width],
        preferred_element_type=jnp.float32,
    ).astype(jnp.bfloat16)
    rows_in = rows_in.reshape(blocks * capacity, width)
    gate_pre = jnp.dot(rows_in, gate, preferred_element_type=jnp.float32)
    up_pre = jnp.dot(rows_in, up, preferred_element_type=jnp.float32)
    glu_part = jnp.minimum(gate_pre, 7.0)
    lin_part = jnp.clip(up_pre, -7.0, 7.0)
    hidden = (glu_part * jax.nn.sigmoid(1.702 * glu_part) * (lin_part + 1.0)).astype(jnp.bfloat16)
    outs = jnp.dot(hidden, down, preferred_element_type=jnp.float32).astype(jnp.bfloat16)
    back = jnp.where(picks, shares[:, None, :], 0).astype(jnp.bfloat16)
    return jnp.einsum(
        "bct,bcd->btd",
        back,
        outs.reshape(blocks, capacity, width),
        preferred_element_type=jnp.float32,
    ).astype(jnp.bfloat16)


def per_device(
    queries_a,
    keys_a,
    values_a,
    queries_b,
    keys_b,
    values_b,
    lambdas,
    head_gain_a,
    head_gain_b,
    out_a,
    out_b,
    residual,
    gain_mix,
    gain_pre,
    gain_post,
    routes,
    route_weights,
    expert_gate,
    expert_up,
    expert_down,
):
    length = queries_a.shape[0]
    heads_a = queries_a.shape[2] // DA
    heads_b = queries_b.shape[2] // DB
    head_slot = lax.axis_index("tp")
    seq_slot = lax.axis_index("sp")
    lambda_a = lax.dynamic_slice_in_dim(lambdas, head_slot * heads_a, heads_a)
    lambda_b = lax.dynamic_slice_in_dim(lambdas, HA + head_slot * heads_b, heads_b)
    experts, tps = lax.axis_size("sp"), lax.axis_size("tp")
    chips = experts // CORES
    own = jnp.concatenate(
        [keys_a.reshape(length, -1), values_a, keys_b.reshape(length, -1), values_b], 1
    )
    queries = jnp.concatenate([queries_a.reshape(length, -1), spread_pairs(queries_b, heads_b)], 1)
    heads_out = attend_blocks(
        queries,
        own,
        jnp.concatenate([lambda_a, lambda_b])[None],
        head_gain_a[None],
        head_gain_b[None],
        chips,
        heads_a,
        heads_b,
    )
    cut = heads_a * 2 * DA
    mixed = (
        jnp.dot(heads_out[:, :cut], out_a, preferred_element_type=jnp.float32)
        + jnp.dot(heads_out[:, cut:], out_b, preferred_element_type=jnp.float32)
    ).astype(jnp.bfloat16)
    mixed_rows = share_rows(mixed.reshape(tps, length // tps, -1), tps)
    after_mix = (residual.astype(jnp.float32) + rms_norm(mixed_rows, gain_mix)).astype(jnp.bfloat16)
    normed = rms_norm(after_mix.astype(jnp.float32), gain_pre).astype(jnp.bfloat16)
    sub_rows = residual.shape[0]
    top_count = routes.shape[1]
    capacity = min(sub_rows, (5 * sub_rows * top_count + 4 * experts - 1) // (4 * experts))
    width = residual.shape[1]
    extra = -(-experts // 128) * 128
    shares = jnp.sum(
        jnp.where(
            routes[:, :, None] == jnp.arange(extra, dtype=jnp.int32)[None, None, :],
            route_weights[:, :, None],
            0.0,
        ),
        1,
    ).astype(jnp.bfloat16)
    gathered = gather_rows(jnp.concatenate([normed, shares], 1), chips, tps)
    parts = expert_parts(
        gathered, seq_slot, experts, capacity, width, (expert_gate[0], expert_up[0], expert_down[0])
    )
    routed = scatter_rows(parts, chips, tps)
    return (after_mix.astype(jnp.float32) + rms_norm(routed, gain_post)).astype(jnp.bfloat16)


def solution(mesh):
    in_specs = (
        P(("grp", "sp"), None, "tp"),
        P(("grp", "sp"), None, "tp"),
        P(("grp", "sp"), "tp"),
        P(("grp", "sp"), None, "tp"),
        P(("grp", "sp"), None, "tp"),
        P(("grp", "sp"), "tp"),
        P(),
        P(),
        P(),
        P("tp", None),
        P("tp", None),
        P(("grp", "sp", "tp"), None),
        P(),
        P(),
        P(),
        P(("grp", "sp", "tp"), None),
        P(("grp", "sp", "tp"), None),
        P("sp", None, "tp"),
        P("sp", None, "tp"),
        P("sp", "tp", None),
    )
    out_specs = P(("grp", "sp", "tp"), None)
    return jax.shard_map(
        per_device, mesh=mesh, in_specs=in_specs, out_specs=out_specs, check_vma=False
    )
```
